128 devices in a mesh: sp: 64 (over z, y, x), tp: 2 (over core).
Axes of the slice: x: 4, y: 4, z: 4, core: 2. Of those that a mesh axis runs over, the one named last changes fastest.
Arguments:
- mid_rows: bfloat16 [8192, 2048], P(('sp', 'tp')), may hold values from -6 to 6
- cotangent: bfloat16 [8192, 2048], P(('sp', 'tp')), may hold values from -24 to 24
- route_experts: int32 [8192, 2], P(('sp', 'tp')), may hold values from 0 to 63, as said below
- route_weights: float32 [8192, 2], P(('sp', 'tp')), may hold values from 0.05 to 0.6
- gate_weight: bfloat16 [64, 2048, 1024], P('sp', None, 'tp'), may hold values from -0.125 to 0.125
- up_weight: bfloat16 [64, 2048, 1024], P('sp', None, 'tp'), may hold values from -0.125 to 0.125
- down_weight: bfloat16 [64, 1024, 2048], P('sp', 'tp'), may hold values from -0.1875 to 0.1875
- out_weight: bfloat16 [2048, 2048], P(None, 'tp'), may hold values from -0.125 to 0.125
- queries: bfloat16 [8192, 1024], P('sp', 'tp'), may hold values from -6 to 6
- key_rows: bfloat16 [8192, 1024], P('sp', 'tp'), may hold values from -6 to 6
- value_rows: bfloat16 [8192, 2048], P('sp', 'tp'), may hold values from -6 to 6
- log_decay: float32 [8192, 1024], P('sp', 'tp'), may hold values from -1 to 0
Outputs:
- gate_gradient: bfloat16 [64, 2048, 1024], P('sp', None, 'tp')
- up_gradient: bfloat16 [64, 2048, 1024], P('sp', None, 'tp')
- down_gradient: bfloat16 [64, 1024, 2048], P('sp', 'tp')
- out_gradient: float32 [2048, 2048], P('sp', 'tp')
- query_gradient: bfloat16 [8192, 1024], P('sp', 'tp')
- key_gradient: bfloat16 [8192, 1024], P('sp', 'tp')
- value_gradient: bfloat16 [8192, 2048], P('sp', 'tp')
- decay_gradient: float32 [8192, 1024], P('sp', 'tp')
The draws below stay inside these ranges and needn't reach their ends.
Inputs may be any that keep to these rules, and one draw needn't show every extreme that they name: `route_experts`: each row names two different experts of one group: both lie among the same 16 consecutive numbers starting at a multiple of 16. Among the rows of one device, no expert is named more than 4 times, and one expert exactly 4 times.
All inputs are finite; a program needn't handle non-finite values.
Results may differ from the reference program's by a relative error of at most 0.0058.
Values may be sent and summed in bfloat16 or wider, within the bound.
No kernel may reach another device: no remote copies, remote signals or barrier semaphores. Data moves between devices by JAX's collectives and lax.ppermute only.
A program may use at most 192 MiB of HBM per device.

```python
import math
import jax
import jax.numpy as jnp
from jax import lax

D = 2048
HEADS = 8
DK = 128
DV = 256
KEY_CHANNELS = 1024
VW = 2048
DE = 1024
GROUPS = 4
BLOCK = 64
TOK_DEV = 128
SEQUENCE_TOKENS = 8192
ROWS = 64
EXPERTS = 64
CAP = 4


def route_block(block_key):
    per_group = EXPERTS // GROUPS
    half_rows = ROWS // 2
    first_key, second_key, third_key, fourth_key = jax.random.split(block_key, 4)
    token_position = jnp.arange(ROWS, dtype=jnp.int32)
    heavy = token_position < half_rows
    cut_points = jax.random.randint(fourth_key, (2,), 0, half_rows + 1).astype(jnp.int32)
    lower_cut = jnp.minimum(cut_points[0], cut_points[1])
    upper_cut = jnp.maximum(cut_points[0], cut_points[1])
    spare = token_position - half_rows
    other_group = jnp.where(spare < lower_cut, 1, jnp.where(spare < upper_cut, 2, 3)).astype(jnp.int32)
    other_start = jnp.where(other_group == 1, 0, jnp.where(other_group == 2, lower_cut, upper_cut)).astype(jnp.int32)
    group = jnp.where(heavy, 0, other_group).astype(jnp.int32)
    group_rank = jnp.where(heavy, token_position, spare - other_start).astype(jnp.int32)
    local_first = group_rank % per_group
    local_second = (group_rank + 1) % per_group
    group_order = jax.random.permutation(first_key, GROUPS).astype(jnp.int32)
    local_keys = jax.random.split(second_key, GROUPS)
    local_order = jax.vmap(jax.random.permutation, in_axes=(0, None))(local_keys, per_group).astype(jnp.int32)
    target = group_order[group]
    expert_first = target * per_group + local_order[group, local_first]
    expert_second = target * per_group + local_order[group, local_second]
    paired = jnp.stack([expert_first, expert_second], axis=1)
    shuffle = jax.random.permutation(third_key, ROWS)
    return paired[shuffle].astype(jnp.int32)


def draw_route_experts(key, part):
    block_total = SEQUENCE_TOKENS // ROWS
    block_keys = jax.random.split(jax.random.fold_in(key, 11), block_total)
    return jax.vmap(route_block)(block_keys).reshape(SEQUENCE_TOKENS, 2).astype(jnp.int32)


def draw_log_decay(key, part):
    random_subkeys = jax.random.split(jax.random.fold_in(key, 23), 7)
    fast_share = 0.5
    fast_channel = jax.random.bernoulli(random_subkeys[0], fast_share, (KEY_CHANNELS,))
    slow_rate = jnp.exp(jax.random.uniform(random_subkeys[1], (KEY_CHANNELS,), jnp.float32, jnp.log(0.1), 0.0)) * (0.5 / SEQUENCE_TOKENS)
    fast_rate = jax.random.uniform(random_subkeys[2], (KEY_CHANNELS,), jnp.float32, 0.01, 1.0 / 30.0)
    channel_decay_rate = jnp.where(fast_channel, fast_rate, slow_rate)
    device_multiplier = jnp.exp(jax.random.uniform(random_subkeys[3], (SEQUENCE_TOKENS // TOK_DEV,), jnp.float32, jnp.log(0.5), 0.0))
    device_multiplier = jnp.repeat(device_multiplier, TOK_DEV)
    random_noise = jax.random.uniform(random_subkeys[4], (SEQUENCE_TOKENS, KEY_CHANNELS), jnp.float32, 0.5, 1.5)
    spike_location = jax.random.randint(random_subkeys[5], (2,), 0, SEQUENCE_TOKENS)
    spike_magnitude = jax.random.uniform(random_subkeys[6], (2, KEY_CHANNELS), jnp.float32, jnp.log(0.5), jnp.log(0.8))
    token_position = jnp.arange(SEQUENCE_TOKENS)
    spike_value = jnp.where(token_position[:, None] == spike_location[0], spike_magnitude[0][None, :], 0.0)
    spike_value = spike_value + jnp.where(token_position[:, None] == spike_location[1], spike_magnitude[1][None, :], 0.0)
    return (spike_value - channel_decay_rate[None, :] * device_multiplier[:, None] * random_noise).astype(jnp.float32)


def spiked(values, key, source, target, blocks, factor):
    def block_of(dim):
        return (jnp.arange(values.shape[dim]) // (values.shape[dim] // blocks)).reshape((-1,) + (1,) * (values.ndim - 1 - dim))

    one_side = jax.random.permutation(key, blocks)[block_of(target)]
    other_side = (block_of(target) + blocks // 2) % blocks
    return jnp.where((block_of(source) == one_side) | (block_of(source) == other_side), factor * values, values)


def levels(stream_key, shape, cuts, smallest, high):
    def one(position, parts):
        draws = jax.random.uniform(jax.random.fold_in(jax.random.fold_in(stream_key, 6), position), (parts,), jnp.float32, smallest / len(cuts), high / len(cuts))
        return jnp.repeat(jnp.exp(draws), shape[position] // parts).reshape((-1,) + (1,) * (len(shape) - position - 1))

    gain = one(*cuts[0])
    for cut in cuts[1:]:
        gain = gain * one(*cut)
    return gain


def gaussian(stream_key, shape, spread, reach, cuts=(), kind=jnp.bfloat16):
    values = jax.random.normal(stream_key, shape, jnp.float32) * spread
    if len(cuts) > 0:
        values = levels(stream_key, shape, cuts, -0.22, 0.18) * values
    return jnp.clip(values, min=-reach, max=reach).astype(kind)


def heavy_noise(own_key, dims, scale, bound, cuts, heavy, held_as=jnp.bfloat16):
    result = scale * jax.random.normal(own_key, dims, jnp.float32)
    if cuts:
        result = result * levels(own_key, dims, cuts, -0.22, 0.18)
    return jnp.clip(spiked(result, jax.random.fold_in(own_key, 3), *heavy), -bound, bound).astype(held_as)


def setup_inputs(seed: int = 0) -> dict:
    arg_keys = jax.random.split(jax.random.key(seed), 13)
    return {
        "mid_rows": gaussian(arg_keys[0], (SEQUENCE_TOKENS, D), 1.0, 6.0, ((0, 128),)),
        "cotangent": heavy_noise(arg_keys[1], (SEQUENCE_TOKENS, D), 1.0, 24.0, ((0, 128),), (0, 1, 128, 5.5)),
        "route_experts": draw_route_experts(jax.random.fold_in(arg_keys[12], 71), 0),
        "route_weights": jnp.clip(jnp.exp(math.log(0.6) - 2.4849067 * jax.random.uniform(arg_keys[3], (SEQUENCE_TOKENS, 2), jnp.float32) ** levels(arg_keys[3], (SEQUENCE_TOKENS, 2), ((0, 128),), -0.2, 0.2)), 0.05, 0.6),
        "gate_weight": gaussian(arg_keys[4], (EXPERTS, D, DE), D ** -0.5, 0.125, ((0, 64), (2, 2))),
        "up_weight": gaussian(arg_keys[5], (EXPERTS, D, DE), D ** -0.5, 0.125, ((0, 64), (2, 2))),
        "down_weight": gaussian(arg_keys[6], (EXPERTS, DE, D), DE ** -0.5, 0.1875, ((0, 64), (1, 2))),
        "out_weight": gaussian(arg_keys[7], (D, VW), VW ** -0.5, 0.125, ((1, 2),)),
        "queries": gaussian(arg_keys[8], (SEQUENCE_TOKENS, KEY_CHANNELS), 1.0, 6.0, ((0, 64), (1, 2))),
        "key_rows": gaussian(arg_keys[9], (SEQUENCE_TOKENS, KEY_CHANNELS), 1.0, 6.0, ((0, 64), (1, 2))),
        "value_rows": gaussian(arg_keys[10], (SEQUENCE_TOKENS, VW), 1.0, 6.0, ((0, 64), (1, 2))),
        "log_decay": draw_log_decay(jax.random.fold_in(arg_keys[12], 71), 0),
    }


precise = lax.Precision.HIGHEST
epsilon = 1e-06
contract_rows = (((0,), (0,)), ((), ()))
contract_cols = (((1,), (1,)), ((), ()))

def silu_parts(pre_gate):
    gate_sigmoid = jax.nn.sigmoid(pre_gate)
    gate_swish = pre_gate * gate_sigmoid
    gate_slope = gate_sigmoid * (1.0 + pre_gate * (1.0 - gate_sigmoid))
    return (gate_swish, gate_slope)

def mixer_normed(query_float, key_float, value_float, decay_float):
    block_count = SEQUENCE_TOKENS // BLOCK
    query_blocks = query_float.reshape(block_count, BLOCK, HEADS, DK) * DK ** (-0.5)
    key_blocks = key_float.reshape(block_count, BLOCK, HEADS, DK)
    value_blocks = value_float.reshape(block_count, BLOCK, HEADS, DV)
    decay_blocks = decay_float.reshape(block_count, BLOCK, HEADS, DK)
    lower_mask = jnp.tril(jnp.ones((BLOCK, BLOCK), jnp.float32))

    def advance(carry_state, inputs):
        query_block, key_block, value_block, decay_block = inputs
        running_log = jnp.cumsum(decay_block, axis=0)
        block_log = running_log[-1]
        query_decayed = query_block * jnp.exp(running_log)
        key_inverse = key_block * jnp.exp(-running_log)
        key_to_end = key_block * jnp.exp(block_log[None] - running_log)
        scores = jnp.einsum('ihc,jhc->hij', query_decayed, key_inverse, precision=precise) * lower_mask
        raw_out = jnp.einsum('hij,jhv->ihv', scores, value_block, precision=precise)
        raw_out = raw_out + jnp.einsum('ihc,hcv->ihv', query_decayed, carry_state, precision=precise)
        new_state = jnp.exp(block_log)[:, :, None] * carry_state + jnp.einsum('jhc,jhv->hcv', key_to_end, value_block, precision=precise)
        return (new_state, raw_out)
    zero_state = jnp.zeros((HEADS, DK, DV), jnp.float32)
    final_state, raw_out = lax.scan(advance, zero_state, (query_blocks, key_blocks, value_blocks, decay_blocks))
    inverse_root = lax.rsqrt(lax.optimization_barrier(jnp.mean(raw_out * raw_out, axis=-1, keepdims=True)) + epsilon)
    return (raw_out * inverse_root).reshape(SEQUENCE_TOKENS, HEADS * DV)

def reference(mid_rows, cotangent, route_experts, route_weights, gate_weight, up_weight, down_weight, out_weight, queries, key_rows, value_rows, log_decay):
    senders = SEQUENCE_TOKENS // ROWS
    slots_total = senders * CAP
    sender_picks = route_experts.reshape(senders, 2 * ROWS)
    one_hot = (sender_picks[:, :, None] == jnp.arange(EXPERTS, dtype=jnp.int32)[None, None, :]).astype(jnp.int32)
    slot_rank = lax.optimization_barrier(jnp.sum((jnp.cumsum(one_hot, axis=1) - one_hot) * one_hot, axis=2))
    slot_index = (jnp.arange(senders, dtype=jnp.int32)[:, None] * CAP + slot_rank).reshape(-1).astype(jnp.int32)
    flat_expert = sender_picks.reshape(-1)
    table = jnp.full((EXPERTS, slots_total), -1, jnp.int32).at[flat_expert, slot_index].set(jnp.arange(2 * SEQUENCE_TOKENS, dtype=jnp.int32))
    flat_weight = route_weights.reshape(-1)
    half_width = DE // 2

    def one_expert(inputs):
        gate_expert, up_expert, down_expert, entries = inputs
        live_slot = entries >= 0
        entry_index = jnp.maximum(entries, 0)
        token_index = entry_index // 2
        rows_in = jnp.where(live_slot[:, None], mid_rows[token_index], jnp.zeros((), jnp.bfloat16))
        scaled = jnp.where(live_slot[:, None], flat_weight[entry_index][:, None] * cotangent[token_index].astype(jnp.float32), 0.0).astype(jnp.bfloat16)
        pre_gate = jnp.dot(rows_in, gate_expert, preferred_element_type=jnp.float32)
        pre_up = jnp.dot(rows_in, up_expert, preferred_element_type=jnp.float32)
        gate_swish, gate_slope = silu_parts(pre_gate)
        hidden = (gate_swish * pre_up).astype(jnp.bfloat16)
        back_hidden = lax.dot_general(scaled, down_expert, contract_cols, preferred_element_type=jnp.float32)
        back_gate = (back_hidden * pre_up * gate_slope).astype(jnp.bfloat16)
        back_up = (back_hidden * gate_swish).astype(jnp.bfloat16)
        gate_total = lax.dot_general(rows_in, back_gate, contract_rows, preferred_element_type=jnp.float32).astype(jnp.bfloat16)
        up_total = lax.dot_general(rows_in, back_up, contract_rows, preferred_element_type=jnp.float32).astype(jnp.bfloat16)
        down_total = lax.dot_general(hidden, scaled, contract_rows, preferred_element_type=jnp.float32).astype(jnp.bfloat16)
        first_half = lax.dot_general(back_gate[:, :half_width], gate_expert[:, :half_width], contract_cols, preferred_element_type=jnp.float32)
        first_half = first_half + lax.dot_general(back_up[:, :half_width], up_expert[:, :half_width], contract_cols, preferred_element_type=jnp.float32)
        second_half = lax.dot_general(back_gate[:, half_width:], gate_expert[:, half_width:], contract_cols, preferred_element_type=jnp.float32)
        second_half = second_half + lax.dot_general(back_up[:, half_width:], up_expert[:, half_width:], contract_cols, preferred_element_type=jnp.float32)
        first_round, second_round = lax.optimization_barrier((first_half.astype(jnp.bfloat16), second_half.astype(jnp.bfloat16)))
        expert_rows = (first_round.astype(jnp.float32) + second_round.astype(jnp.float32)).astype(jnp.bfloat16)
        return (gate_total, up_total, down_total, expert_rows)
    gate_total, up_total, down_total, expert_rows = lax.map(one_expert, (gate_weight, up_weight, down_weight, table))
    picked = expert_rows[flat_expert, slot_index].reshape(SEQUENCE_TOKENS, 2, D)
    token_back = (cotangent.astype(jnp.float32) + picked[:, 0].astype(jnp.float32) + picked[:, 1].astype(jnp.float32)).astype(jnp.bfloat16)
    normed, pullback = jax.vjp(mixer_normed, queries.astype(jnp.float32), key_rows.astype(jnp.float32), value_rows.astype(jnp.float32), log_decay)
    normed_rows = normed.astype(jnp.bfloat16)
    out_gradient = lax.dot_general(token_back, normed_rows, contract_rows, preferred_element_type=jnp.float32)
    back_normed = jnp.dot(token_back, out_weight, preferred_element_type=jnp.float32)
    query_back, key_back, value_back, decay_back = pullback(back_normed)
    return (gate_total, up_total, down_total, out_gradient, query_back.astype(jnp.bfloat16), key_back.astype(jnp.bfloat16), value_back.astype(jnp.bfloat16), decay_back)
```

```python
import functools

import jax
import jax.numpy as jnp
from jax import lax
from jax.experimental import pallas as pl
from jax.experimental.pallas import tpu as pltpu
from jax.sharding import Mesh
from jax.sharding import PartitionSpec as P

DK = 128
DV = 256
SP = ("sp_0", "sp_1", "sp_2")
SP_TP = ("sp_0", "sp_1", "sp_2", "tp")
ROWS = 64
D = 2048
HALF = 1024
HID = 512
HEADS = 4
TOK = 128
NDEV = 64
SW = DV + 128
MSG = SW + D
RET = DV + HALF
SCALE = DK**-0.5

f32 = jnp.float32
bf16 = jnp.bfloat16
epsilon = 1e-06


def dot(a, b, ca, cb, high=False):
    return lax.dot_general(
        a,
        b,
        (((ca,), (cb,)), ((), ())),
        precision=lax.Precision.HIGHEST if high else None,
        preferred_element_type=f32,
    )


def call(kernel, out_shape, args, specs=None, scratch=(), flops=0, name=None):
    specs = specs or [None] * len(args)
    vmem = pl.BlockSpec(memory_space=pltpu.VMEM)
    many = isinstance(out_shape, (list, tuple))
    return pl.pallas_call(
        kernel,
        out_shape=out_shape,
        in_specs=[s or vmem for s in specs],
        out_specs=[vmem] * len(out_shape) if many else vmem,
        scratch_shapes=list(scratch),
        compiler_params=pltpu.CompilerParams(vmem_limit_bytes=56 * 1024 * 1024),
        cost_estimate=pl.CostEstimate(flops=flops, transcendentals=0, bytes_accessed=1 << 20),
        name=name,
    )(*args)


SMEM = pl.BlockSpec(memory_space=pltpu.SMEM)
ANY = pl.BlockSpec(memory_space=pl.ANY)


def tri(lower, strict=False):
    i = lax.broadcasted_iota(jnp.int32, (TOK, TOK), 0)
    j = lax.broadcasted_iota(jnp.int32, (TOK, TOK), 1)
    return (i >= j) if lower else (i <= j)


def head_cols(ref, h, width):
    return ref[:, h * width : (h + 1) * width].astype(f32)


def state_kernel(k_ref, v_ref, a_ref, msg_ref):
    lower = tri(True).astype(f32)
    ones = jnp.ones((TOK, 128), f32)
    lane = lax.broadcasted_iota(jnp.int32, (DK, 128), 1)
    for h in range(HEADS):
        a = head_cols(a_ref, h, DK)
        r = dot(lower, a, 1, 0, True)
        ke = head_cols(k_ref, h, DK) * jnp.exp(r[TOK - 1 :, :] - r)
        s = dot(ke, head_cols(v_ref, h, DV), 0, 0, True)
        rows = slice(h * DK, (h + 1) * DK)
        msg_ref[rows, 0:DV] = s.astype(bf16)
        col = dot(a, ones, 0, 0, True)
        hi = col.astype(bf16).astype(f32)
        mid = (col - hi).astype(bf16).astype(f32)
        lo = col - hi - mid
        part = jnp.where(lane == 0, hi, jnp.where(lane == 1, mid, jnp.where(lane == 2, lo, 0.0)))
        msg_ref[rows, DV:SW] = part.astype(bf16)


def pack_kernel(core_ref, route_ref, route2_ref, mid_ref, mid2_ref, cot_ref, cot2_ref, st_ref, out_ref, pick_ref):
    core = core_ref[0]
    lane = lax.broadcasted_iota(jnp.int32, (ROWS, NDEV), 1).astype(f32)
    ti = lax.broadcasted_iota(jnp.int32, (ROWS, ROWS), 0)
    tj = lax.broadcasted_iota(jnp.int32, (ROWS, ROWS), 1)
    before = (ti > tj).astype(f32)
    si = lax.broadcasted_iota(jnp.int32, (8 * NDEV, NDEV), 0)
    se = lax.broadcasted_iota(jnp.int32, (8 * NDEV, NDEV), 1)
    expand = (si // 8 == se).astype(f32)
    slot = (si % 4 + 1).astype(f32)
    owner = (si % 8) // 4

    def picks(ref, which):
        e1 = (ref[:, 0:1] == lane).astype(f32)
        e2 = (ref[:, 1:2] == lane).astype(f32)
        both = e1 + e2
        rank = both * (dot(before, both, 1, 0, True) + 1.0)
        weight = e1 * ref[:, 2:3] + e2 * ref[:, 3:4]
        found = dot(expand, rank, 1, 1, True)
        pick = jnp.where((found == slot) & (owner == which), 1.0, 0.0)
        w = jnp.sum(pick * dot(expand, weight, 1, 1, True), axis=1, keepdims=True)
        return pick, w

    own, w_own = picks(route_ref, core)
    other, w_other = picks(route2_ref, 1 - core)
    pick_ref[:, 0:ROWS] = own.astype(bf16)
    pick_ref[:, ROWS:] = other.astype(bf16)
    out_ref[:, 0:SW] = st_ref[...]
    own = own.astype(bf16)
    other = other.astype(bf16)

    @pl.when(core == 0)
    def _():
        rows = dot(own, mid_ref[...], 1, 0) + dot(other, mid2_ref[...], 1, 0)
        out_ref[:, SW:] = rows.astype(bf16)

    @pl.when(core == 1)
    def _():
        rows = dot(own, cot_ref[...], 1, 0) + dot(other, cot2_ref[...], 1, 0)
        out_ref[:, SW:] = (rows * (w_own + w_other)).astype(bf16)


def scan_kernel(msg_ref, dec_ref, out_ref, x_ref, d_ref, y_ref, *, reverse):
    x_ref[...] = msg_ref[:, 0:DV].astype(f32)
    log = jnp.sum(dec_ref[...].astype(f32), axis=1, keepdims=True)
    d_ref[...] = jnp.broadcast_to(jnp.exp(log), (8 * NDEV, DV))
    state = jnp.zeros((8, DV), f32)
    for n in range(NDEV):
        p = NDEV - 1 - n if reverse else n
        rows = slice(8 * p, 8 * p + 8)
        y_ref[rows, :] = state
        state = d_ref[rows, :] * state + x_ref[rows, :]
    out_ref[...] = y_ref[...].astype(bf16)


def expert_kernel(
    core_ref, mine_ref, theirs_ref, gate_ref, up_ref, down_ref,
    keep_ref, send_ref, rows_ref, scaled_ref, hidden_ref, bg_ref, bu_ref,
    sems,
):
    core = core_ref[0]
    part = (slice(None), pl.ds(SW, D))

    def fetch(a_ref, b_ref):
        first = pltpu.make_async_copy(a_ref.at[part], rows_ref, sems.at[0])
        second = pltpu.make_async_copy(b_ref.at[part], scaled_ref, sems.at[1])
        first.start()
        second.start()
        first.wait()
        second.wait()

    @pl.when(core == 0)
    def _():
        fetch(mine_ref, theirs_ref)

    @pl.when(core == 1)
    def _():
        fetch(theirs_ref, mine_ref)

    x = rows_ref[...]
    pre_gate = dot(x, gate_ref[...], 1, 0)
    pre_up = dot(x, up_ref[...], 1, 0)
    sig = 1.0 / (1.0 + jnp.exp(-pre_gate))
    swish = pre_gate * sig
    slope = sig * (1.0 + pre_gate * (1.0 - sig))
    hidden_ref[...] = (swish * pre_up).astype(bf16)
    back = dot(scaled_ref[...], down_ref[...], 1, 1)
    bg = (back * pre_up * slope).astype(bf16)
    bu = (back * swish).astype(bf16)
    bg_ref[...] = bg
    bu_ref[...] = bu

    def half(c):
        cols = pl.ds(pl.multiple_of(c * HALF, HALF), HALF)
        total = dot(bg, gate_ref[cols, :], 1, 1) + dot(bu, up_ref[cols, :], 1, 1)
        return total.astype(bf16)

    send_ref[...] = half(1 - core)
    keep_ref[...] = half(core)


def return_kernel(keep_ref, got_ref, state_ref, out_ref):
    out_ref[:, 0:DV] = state_ref[...]
    out_ref[:, DV:] = (keep_ref[...].astype(f32) + got_ref[...].astype(f32)).astype(bf16)


def combine_kernel(core_ref, pick_ref, ret_ref, cot_ref, cot2_ref, out_ref):
    core = core_ref[0]
    rows = ret_ref[:, DV:]
    cols = pl.ds(pl.multiple_of(core * HALF, HALF), HALF)

    def put(lanes, cot, which):
        total = dot(pick_ref[:, lanes], rows, 0, 0) + cot[:, cols].astype(f32)
        out_ref[pl.ds(pl.multiple_of(which * ROWS, ROWS), ROWS), :] = total.astype(bf16)

    put(slice(0, ROWS), cot_ref, core)
    put(slice(ROWS, 2 * ROWS), cot2_ref, 1 - core)


def forward_parts(q_ref, k_ref, v_ref, a_ref, h):
    lower = tri(True)
    r = dot(lower.astype(f32), head_cols(a_ref, h, DK), 1, 0, True)
    mid = r[TOK // 2 : TOK // 2 + 1, :]
    up = jnp.exp(r - mid)
    down = jnp.exp(mid - r)
    q = head_cols(q_ref, h, DK) * SCALE
    k = head_cols(k_ref, h, DK)
    v = head_cols(v_ref, h, DV)
    qd = q * up
    ki = k * down
    scores = jnp.where(lower, dot(qd, ki, 1, 1, True), 0.0)
    return r, up, down, q, k, v, qd, ki, scores


def mixer_kernel(
    core_ref, mine_ref, theirs_ref, w_ref, q_ref, k_ref, v_ref, a_ref, ret_ref,
    msg_ref, og_ref, braw_ref,
):
    core = core_ref[0]
    mine = mine_ref[...]
    theirs = theirs_ref[...]
    row_mine = pl.multiple_of(core * HALF, HALF)
    row_theirs = pl.multiple_of((1 - core) * HALF, HALF)
    braw_ref[...] = dot(mine, w_ref[pl.ds(row_mine, HALF), :], 1, 0) + dot(
        theirs, w_ref[pl.ds(row_theirs, HALF), :], 1, 0
    )
    for i in range(2):
        cols = slice(i * HID, (i + 1) * HID)
        og_ref[2 * core + i, :, 0:HID] = mine[:, cols]
        og_ref[2 * (1 - core) + i, :, 0:HID] = theirs[:, cols]
    for h in range(HEADS):
        r, up, down, q, k, v, qd, ki, scores = forward_parts(q_ref, k_ref, v_ref, a_ref, h)
        rows = slice(h * DK, (h + 1) * DK)
        cols = slice(h * DV, (h + 1) * DV)
        s_in = ret_ref[rows, 0:DV].astype(f32)
        q_abs = q * jnp.exp(r)
        raw = dot(scores, v, 1, 0, True) + dot(q_abs, s_in, 1, 0, True)
        inv = lax.rsqrt(jnp.mean(raw * raw, axis=1, keepdims=True) + epsilon)
        normed = raw * inv
        bn = braw_ref[:, cols]
        braw = inv * (bn - normed * jnp.mean(bn * normed, axis=1, keepdims=True))
        braw_ref[:, cols] = braw
        msg_ref[rows, :] = dot(q_abs, braw, 0, 0, True).astype(bf16)
        normed = normed.astype(bf16)
        for z in range(4):
            og_ref[z, :, HID + h * DV : HID + (h + 1) * DV] = normed


def local_kernel(
    q_ref, k_ref, v_ref, a_ref, ret_ref, braw_ref, qo_ref, dk_ref, dv_ref, dd_ref
):
    for h in range(HEADS):
        r, up, down, q, k, v, qd, ki, scores = forward_parts(q_ref, k_ref, v_ref, a_ref, h)
        rows = slice(h * DK, (h + 1) * DK)
        keys = slice(h * DK, (h + 1) * DK)
        cols = slice(h * DV, (h + 1) * DV)
        s_in = ret_ref[rows, 0:DV].astype(f32)
        braw = braw_ref[:, cols]
        vd = jnp.where(tri(True), dot(braw, v, 1, 1, True), 0.0)
        dq = up * dot(vd, ki, 1, 0, True) + jnp.exp(r) * dot(braw, s_in, 1, 1, True)
        dk = down * dot(vd, qd, 0, 0, True)
        dv = dot(scores, braw, 0, 0, True)
        qo_ref[:, keys] = (dq * SCALE).astype(bf16)
        dk_ref[:, keys] = dk
        dv_ref[:, cols] = dv
        dd_ref[:, keys] = q * dq - k * dk


def final_kernel(
    k_ref, v_ref, a_ref, ret_ref, fut_ref, dk_ref, dv_ref, dd_ref, ko_ref, vo_ref, do_ref
):
    lower = tri(True).astype(f32)
    upper = tri(False).astype(f32)
    ones = jnp.ones((TOK, 128), f32)
    ones_row = jnp.ones((8, DV), f32)
    for h in range(HEADS):
        rows = slice(h * DK, (h + 1) * DK)
        keys = slice(h * DK, (h + 1) * DK)
        cols = slice(h * DV, (h + 1) * DV)
        a = head_cols(a_ref, h, DK)
        k = head_cols(k_ref, h, DK)
        v = head_cols(v_ref, h, DV)
        r = dot(lower, a, 1, 0, True)
        to_end = jnp.exp(r[TOK - 1 :, :] - r)
        ke = k * to_end
        fut = fut_ref[rows, :].astype(f32)
        s_in = ret_ref[rows, 0:DV].astype(f32)
        decay = jnp.exp(dot(a, ones, 0, 0, True))[:, 0:1]
        s_end = decay * s_in + dot(ke, v, 0, 0, True)
        cross = dot(ones_row, s_end * fut, 1, 1, True)[0:1, :]
        more = to_end * dot(v, fut, 1, 1, True)
        ko_ref[:, keys] = (dk_ref[:, keys] + more).astype(bf16)
        vo_ref[:, cols] = (dv_ref[:, cols] + dot(ke, fut, 1, 0, True)).astype(bf16)
        back = dd_ref[:, keys] - k * more
        do_ref[:, keys] = dot(upper, back, 1, 0, True) + cross


def outer_kernel(og_ref, out_ref):
    total = dot(og_ref[0, :, 0:HID], og_ref[0, :, HID:], 0, 0)
    for z in range(1, 4):
        total = total + dot(og_ref[z, :, 0:HID], og_ref[z, :, HID:], 0, 0)
    out_ref[...] = total.astype(bf16)


def shape(dims, dtype):
    return jax.ShapeDtypeStruct(dims, dtype)


def swapped(x):
    return lax.ppermute(x, "tp", [(0, 1), (1, 0)])


def exchanged(x, axes, count):
    parts = x.reshape(count, x.shape[0] // count, *x.shape[1:])
    return lax.all_to_all(parts, axes, split_axis=0, concat_axis=0, tiled=True).reshape(x.shape)


def body(
    mid_rows,
    cotangent,
    route_experts,
    route_weights,
    gate_weight,
    up_weight,
    down_weight,
    out_weight,
    queries,
    key_rows,
    value_rows,
    log_decay,
):
    core = lax.axis_index("tp").astype(jnp.int32).reshape(1)
    route = jnp.concatenate([route_experts.astype(f32), route_weights], axis=1)
    mid2, cot2, route2 = swapped(mid_rows), swapped(cotangent), swapped(route)
    gate, up, down = gate_weight[0], up_weight[0], down_weight[0]
    state_msg = call(
        state_kernel, shape((HEADS * DK, SW), bf16), (key_rows, value_rows, log_decay), name="state", flops=1 << 28
    )
    send, pick = call(
        pack_kernel,
        (shape((8 * NDEV, MSG), bf16), shape((8 * NDEV, 2 * ROWS), bf16)),
        (core, route, route2, mid_rows, mid2, cotangent, cot2, state_msg),
        [SMEM] + [None] * 7,
        name="pack",
        flops=1 << 28,
    )
    got = exchanged(send, SP, NDEV)
    theirs = swapped(got)
    scan_scratch = [pltpu.VMEM((8 * NDEV, DV), f32)] * 3
    state_spec = pl.BlockSpec((8 * NDEV, DV), lambda i: (0, 0))
    decay_spec = pl.BlockSpec((8 * NDEV, 128), lambda i: (0, DV // 128))

    def scanned(msg, decays, reverse):
        return pl.pallas_call(
            functools.partial(scan_kernel, reverse=reverse),
            grid=(1,),
            out_shape=shape((8 * NDEV, DV), bf16),
            in_specs=[state_spec, decay_spec],
            out_specs=state_spec,
            scratch_shapes=scan_scratch,
            name="scan",
        )(msg, decays)

    state_in = scanned(got, got, False)
    keep, give, rows_in, scaled, hidden, back_gate, back_up = call(
        expert_kernel,
        (shape((512, HALF), bf16), shape((512, HALF), bf16), shape((512, D), bf16), shape((512, D), bf16))
        + (shape((512, HID), bf16),) * 3,
        (core, got, theirs, gate, up, down),
        [SMEM, ANY, ANY, None, None, None],
        [pltpu.SemaphoreType.DMA((2,))],
        name="expert",
        flops=6 << 30,
    )
    summed = call(
        return_kernel, shape((512, RET), bf16), (keep, swapped(give), state_in), name="returned", flops=1 << 20
    )
    ret = exchanged(summed, SP, NDEV)
    gate_total = dot(rows_in, back_gate, 0, 0).astype(bf16)[None]
    up_total = dot(rows_in, back_up, 0, 0).astype(bf16)[None]
    down_total = dot(hidden, scaled, 0, 0).astype(bf16)[None]
    token_mine = call(
        combine_kernel,
        shape((TOK, HALF), bf16),
        (core, pick, ret, cotangent, cot2),
        [SMEM] + [None] * 4,
        name="combine",
        flops=1 << 26,
    )
    token_theirs = swapped(token_mine)
    back_msg, og, braw = call(
        mixer_kernel,
        (shape((512, DV), bf16), shape((4, TOK, HID + HALF), bf16), shape((TOK, HALF), f32)),
        (core, token_mine, token_theirs, out_weight, queries, key_rows, value_rows, log_decay, ret),
        [SMEM] + [None] * 8,
        name="mixer",
        flops=1 << 30,
    )
    back_got = exchanged(back_msg, SP, NDEV)
    og_got = lax.all_to_all(og, "sp_0", split_axis=0, concat_axis=0, tiled=True)
    query_out, dk_part, dv_part, dd_part = call(
        local_kernel,
        (shape((TOK, 512), bf16), shape((TOK, 512), f32), shape((TOK, HALF), f32), shape((TOK, 512), f32)),
        (queries, key_rows, value_rows, log_decay, ret, braw),
        name="local",
        flops=1 << 30,
    )
    future = exchanged(scanned(back_got, got, True), SP, NDEV)
    outer = call(outer_kernel, shape((512, HALF), bf16), (og_got,), name="outer", flops=1 << 29)
    terms = lax.all_to_all(
        outer.reshape(16, 32, HALF), ("sp_1", "sp_2"), split_axis=0, concat_axis=0, tiled=True
    )
    out_total = terms.astype(f32).sum(axis=0)
    key_out, value_out, decay_out = call(
        final_kernel,
        (shape((TOK, 512), bf16), shape((TOK, HALF), bf16), shape((TOK, 512), f32)),
        (key_rows, value_rows, log_decay, ret, future, dk_part, dv_part, dd_part),
        name="final",
        flops=1 << 29,
    )
    return (gate_total, up_total, down_total, out_total, query_out, key_out, value_out, decay_out)


def solution(mesh):
    split = Mesh(mesh.devices.reshape(4, 4, 4, mesh.shape["tp"]), ("sp_0", "sp_1", "sp_2", "tp"))
    placed = (
        P(SP_TP, None),
        P(SP_TP, None),
        P(SP_TP, None),
        P(SP_TP, None),
        P(SP, None, "tp"),
        P(SP, None, "tp"),
        P(SP, "tp", None),
        P(None, "tp"),
        P(SP, "tp"),
        P(SP, "tp"),
        P(SP, "tp"),
        P(SP, "tp"),
    )
    return jax.shard_map(
        body,
        mesh=split,
        in_specs=placed,
        out_specs=(
            P(SP, None, "tp"),
            P(SP, None, "tp"),
            P(SP, "tp", None),
            P(SP, "tp"),
            P(SP, "tp"),
            P(SP, "tp"),
            P(SP, "tp"),
            P(SP, "tp"),
        ),
        check_vma=False,
    )
```

```python
import functools

import jax
import jax.numpy as jnp
from jax import lax
from jax.experimental import pallas as pl
from jax.experimental.pallas import tpu as pltpu
from jax.sharding import Mesh
from jax.sharding import PartitionSpec as P


DK = 128
DV = 256
SP = ("sp_0", "sp_1", "sp_2")
SP_TP = ("sp_0", "sp_1", "sp_2", "tp")
ROWS = 64
D = 2048
HALF = 1024
HID = 512
HEADS = 4
TOK = 128
NDEV = 64
SW = DV + 128
MSG = SW + D
SCALE = DK**-0.5


f32 = jnp.float32
bf16 = jnp.bfloat16
epsilon = 1e-06


def dot(a, b, ca, cb, high=False):
    return lax.dot_general(
        a,
        b,
        (((ca,), (cb,)), ((), ())),
        precision=lax.Precision.HIGHEST if high else None,
        preferred_element_type=f32,
    )


def fast(dims, dtype):
    return pltpu.VMEM(dims, dtype)


def far_out(dims, dtype):
    return pltpu.HBM(dims, dtype)


SMEM, NEAR, FAR = "s", "n", "f"


def call(kernel, out_shape, args, kinds, scratch=(), flops=0, limit=12, manual=()):
    vmem = pl.BlockSpec(memory_space=pltpu.VMEM)
    specs = {SMEM: pl.BlockSpec(memory_space=pltpu.SMEM), FAR: pl.BlockSpec(memory_space=pl.ANY)}
    spaces = {NEAR: pltpu.VMEM, FAR: pltpu.HBM}
    many = isinstance(out_shape, (list, tuple))
    outs = list(out_shape) if many else [out_shape]
    out_specs = [specs[FAR] if i in manual else vmem for i in range(len(outs))]
    args = [
        pltpu.with_memory_space_constraint(a, spaces[k]) if k in spaces else a for a, k in zip(args, kinds)
    ]
    return pl.pallas_call(
        kernel,
        out_shape=out_shape,
        in_specs=[specs.get(k, vmem) for k in kinds],
        out_specs=out_specs if many else out_specs[0],
        scratch_shapes=list(scratch),
        compiler_params=pltpu.CompilerParams(vmem_limit_bytes=limit * 1024 * 1024),
        cost_estimate=pl.CostEstimate(flops=flops, transcendentals=0, bytes_accessed=1 << 20),
    )(*args)


def tri(lower):
    i = lax.broadcasted_iota(jnp.int32, (TOK, TOK), 0)
    j = lax.broadcasted_iota(jnp.int32, (TOK, TOK), 1)
    return (i >= j) if lower else (i <= j)


def head_cols(ref, h, width):
    return ref[:, h * width : (h + 1) * width].astype(f32)


def state_kernel(k_ref, v_ref, a_ref, msg_ref):
    lower = tri(True).astype(f32)
    ones = jnp.ones((TOK, 128), f32)
    lane = lax.broadcasted_iota(jnp.int32, (DK, 128), 1)
    for h in range(HEADS):
        a = head_cols(a_ref, h, DK)
        r = dot(lower, a, 1, 0, True)
        ke = head_cols(k_ref, h, DK) * jnp.exp(r[TOK - 1 :, :] - r)
        s = dot(ke, head_cols(v_ref, h, DV), 0, 0, True)
        rows = slice(h * DK, (h + 1) * DK)
        msg_ref[rows, 0:DV] = s.astype(bf16)
        col = dot(a, ones, 0, 0, True)
        hi = col.astype(bf16).astype(f32)
        mid = (col - hi).astype(bf16).astype(f32)
        lo = col - hi - mid
        part = jnp.where(lane == 0, hi, jnp.where(lane == 1, mid, jnp.where(lane == 2, lo, 0.0)))
        msg_ref[rows, DV:SW] = part.astype(bf16)


def pack_kernel(
    core_ref, ids_ref, ids2_ref, wts_ref, wts2_ref, mid_ref, mid2_ref, cot_ref, cot2_ref, state_ref,
    out_ref, pick_ref, rows_ref, send_ref, pick_v_ref, sems,
):
    core = core_ref[0]

    @pl.when(core == 0)
    def _():
        pltpu.make_async_copy(mid_ref, rows_ref.at[0:ROWS], sems.at[0]).start()
        pltpu.make_async_copy(mid2_ref, rows_ref.at[ROWS : 2 * ROWS], sems.at[1]).start()

    @pl.when(core == 1)
    def _():
        pltpu.make_async_copy(cot_ref, rows_ref.at[0:ROWS], sems.at[0]).start()
        pltpu.make_async_copy(cot2_ref, rows_ref.at[ROWS : 2 * ROWS], sems.at[1]).start()

    state_out = pltpu.make_async_copy(state_ref, out_ref.at[:, 0:SW], sems.at[7])
    state_out.start()
    expert = lax.broadcasted_iota(jnp.int32, (NDEV, ROWS), 0)
    ti = lax.broadcasted_iota(jnp.int32, (ROWS, ROWS), 0)
    tj = lax.broadcasted_iota(jnp.int32, (ROWS, ROWS), 1)
    before = (ti < tj).astype(bf16)
    si = lax.broadcasted_iota(jnp.int32, (8 * NDEV, NDEV), 0)
    se = lax.broadcasted_iota(jnp.int32, (8 * NDEV, NDEV), 1)
    expand = (si // 8 == se).astype(bf16)
    slot = (si % 4 + 1).astype(f32)
    owner = (si % 8) // 4

    def picks(ids, wts, which):
        e1 = (ids[0:1, :] == expert).astype(f32)
        e2 = (ids[1:2, :] == expert).astype(f32)
        both = e1 + e2
        rank = both * (dot(both.astype(bf16), before, 1, 0) + 1.0)
        weight = e1 * wts[0:1, :] + e2 * wts[1:2, :]
        found = dot(expand, rank.astype(bf16), 1, 0)
        return jnp.where((found == slot) & (owner == which), 1.0, 0.0), weight

    own, weight_own = picks(ids_ref, wts_ref, core)
    other, weight_other = picks(ids2_ref, wts2_ref, 1 - core)
    pick_v_ref[:, 0:ROWS] = own.astype(bf16)
    pick_v_ref[:, ROWS:] = other.astype(bf16)
    pick_out = pltpu.make_async_copy(pick_v_ref, pick_ref, sems.at[2])
    pick_out.start()
    wide = expand.astype(f32)
    w = own * dot(wide, weight_own, 1, 0, True) + other * dot(wide, weight_other, 1, 0, True)
    scale = jnp.where(core == 0, 1.0, jnp.sum(w, axis=1, keepdims=True))
    pltpu.make_async_copy(mid_ref, rows_ref.at[0:ROWS], sems.at[0]).wait()
    pltpu.make_async_copy(mid2_ref, rows_ref.at[ROWS : 2 * ROWS], sems.at[1]).wait()
    outs = []
    for i in range(4):
        cols = slice(i * HID, (i + 1) * HID)
        rows = dot(pick_v_ref[...], rows_ref[:, cols], 1, 0)
        send_ref[:, cols] = (rows * scale).astype(bf16)
        to = out_ref.at[:, SW + i * HID : SW + (i + 1) * HID]
        outs.append(pltpu.make_async_copy(send_ref.at[:, cols], to, sems.at[3 + i]))
        outs[i].start()
    pick_out.wait()
    state_out.wait()
    for c in outs:
        c.wait()


def grads_kernel(
    core_ref, got_ref, other_ref, hidden_ref, bg_ref, bu_ref, gate_ref, up_ref, down_ref, rows_ref, scaled_ref, sems
):
    core = core_ref[0]
    got_ref = got_ref.at[:, SW:MSG]
    other_ref = other_ref.at[:, SW:MSG]

    @pl.when(core == 0)
    def _():
        pltpu.make_async_copy(got_ref, rows_ref, sems.at[0]).start()
        pltpu.make_async_copy(other_ref, scaled_ref, sems.at[1]).start()

    @pl.when(core == 1)
    def _():
        pltpu.make_async_copy(other_ref, rows_ref, sems.at[0]).start()
        pltpu.make_async_copy(got_ref, scaled_ref, sems.at[1]).start()

    pltpu.make_async_copy(got_ref, rows_ref, sems.at[0]).wait()
    pltpu.make_async_copy(got_ref, scaled_ref, sems.at[1]).wait()

    def part(i, carry):
        part = pl.ds(pl.multiple_of(i * HID, HID), HID)
        x = rows_ref[:, part]
        gate_ref[part, :] = dot(x, bg_ref[...], 0, 0).astype(bf16)
        up_ref[part, :] = dot(x, bu_ref[...], 0, 0).astype(bf16)
        down_ref[:, part] = dot(hidden_ref[...], scaled_ref[:, part], 0, 0).astype(bf16)
        return carry

    lax.fori_loop(0, 4, part, 0)


def load_kernel(*refs):
    count = (len(refs) - 1) // 2
    copies = [pltpu.make_async_copy(refs[i], refs[count + i], refs[-1].at[i]) for i in range(count)]
    for c in copies:
        c.start()
    for c in copies:
        c.wait()


def scan_kernel(*refs, reverse):
    got_ref, out_ref, part_ref, x_ref, d_ref, y_ref, sem = refs[-7:]
    copy = pltpu.make_async_copy(got_ref.at[:, 0:SW], part_ref, sem.at[0])
    copy.start()
    copy.wait()
    msg_ref = refs[0] if reverse else part_ref
    x_ref[...] = msg_ref[:, 0:DV].astype(f32)
    log = jnp.sum(part_ref[:, DV:].astype(f32), axis=1, keepdims=True)
    d_ref[...] = jnp.broadcast_to(jnp.exp(log), (8 * NDEV, DV))
    state = jnp.zeros((8, DV), f32)
    for n in range(NDEV):
        p = NDEV - 1 - n if reverse else n
        rows = slice(8 * p, 8 * p + 8)
        y_ref[rows, :] = state
        state = d_ref[rows, :] * state + x_ref[rows, :]
    out_ref[...] = y_ref[...].astype(bf16)


def expert_kernel(
    core_ref, mine_ref, theirs_ref, gate_ref, up_ref, down_ref,
    keep_ref, send_ref, hidden_out, bg_out, bu_out,
    rows_ref, scaled_ref, hidden_ref, bg_ref, bu_ref, sems,
):
    core = core_ref[0]
    mine_ref = mine_ref.at[:, SW:MSG]
    theirs_ref = theirs_ref.at[:, SW:MSG]

    @pl.when(core == 0)
    def _():
        pltpu.make_async_copy(mine_ref, rows_ref, sems.at[0]).start()
        pltpu.make_async_copy(theirs_ref, scaled_ref, sems.at[1]).start()

    @pl.when(core == 1)
    def _():
        pltpu.make_async_copy(theirs_ref, rows_ref, sems.at[0]).start()
        pltpu.make_async_copy(mine_ref, scaled_ref, sems.at[1]).start()

    pltpu.make_async_copy(mine_ref, rows_ref, sems.at[0]).wait()
    pre_gate = dot(rows_ref[...], gate_ref[...], 1, 0)
    pre_up = dot(rows_ref[...], up_ref[...], 1, 0)
    sig = 1.0 / (1.0 + jnp.exp(-pre_gate))
    swish = pre_gate * sig
    slope = sig * (1.0 + pre_gate * (1.0 - sig))
    hidden_ref[...] = (swish * pre_up).astype(bf16)
    hidden_copy = pltpu.make_async_copy(hidden_ref, hidden_out, sems.at[2])
    hidden_copy.start()
    pltpu.make_async_copy(mine_ref, scaled_ref, sems.at[1]).wait()
    back = dot(scaled_ref[...], down_ref[...], 1, 1)
    bg_ref[...] = (back * pre_up * slope).astype(bf16)
    bu_ref[...] = (back * swish).astype(bf16)
    bg_copy = pltpu.make_async_copy(bg_ref, bg_out, sems.at[3])
    bu_copy = pltpu.make_async_copy(bu_ref, bu_out, sems.at[4])
    bg_copy.start()
    bu_copy.start()

    def half(c):
        cols = pl.ds(pl.multiple_of(c * HALF, HALF), HALF)
        total = dot(bg_ref[...], gate_ref[cols, :], 1, 1) + dot(bu_ref[...], up_ref[cols, :], 1, 1)
        return total.astype(bf16)

    send_ref[...] = half(1 - core)
    keep_ref[...] = half(core)
    for c in (hidden_copy, bg_copy, bu_copy):
        c.wait()


def return_kernel(keep_ref, got_ref, out_ref):
    out_ref[...] = (keep_ref[...].astype(f32) + got_ref[...].astype(f32)).astype(bf16)


def combine_kernel(core_ref, pick_ref, ret_ref, cot_ref, cot2_ref, out_ref):
    core = core_ref[0]
    rows = ret_ref[...]
    cols = pl.ds(pl.multiple_of(core * HALF, HALF), HALF)

    def put(lanes, cot, which):
        total = dot(pick_ref[:, lanes], rows, 0, 0) + cot[:, cols].astype(f32)
        out_ref[pl.ds(pl.multiple_of(which * ROWS, ROWS), ROWS), :] = total.astype(bf16)

    put(slice(0, ROWS), cot_ref, core)
    put(slice(ROWS, 2 * ROWS), cot2_ref, 1 - core)


def forward_parts(q_ref, k_ref, v_ref, a_ref, h):
    lower = tri(True)
    r = dot(lower.astype(f32), head_cols(a_ref, h, DK), 1, 0, True)
    mid = r[TOK // 2 : TOK // 2 + 1, :]
    up = jnp.exp(r - mid)
    down = jnp.exp(mid - r)
    q = head_cols(q_ref, h, DK) * SCALE
    k = head_cols(k_ref, h, DK)
    v = head_cols(v_ref, h, DV)
    qd = q * up
    ki = k * down
    scores = jnp.where(lower, dot(qd, ki, 1, 1, True), 0.0)
    return r, up, down, q, k, v, qd, ki, scores


def prior_kernel(q_ref, k_ref, v_ref, a_ref, inner_ref, qabs_ref, ke_ref, toend_ref, sloc_ref):
    for h in range(HEADS):
        r, _, _, q, k, v, _, _, scores = forward_parts(q_ref, k_ref, v_ref, a_ref, h)
        keys = slice(h * DK, (h + 1) * DK)
        inner_ref[:, h * DV : (h + 1) * DV] = dot(scores, v, 1, 0, True)
        qabs_ref[:, keys] = q * jnp.exp(r)
        to_end = jnp.exp(r[TOK - 1 :, :] - r)
        ke = k * to_end
        ke_ref[:, keys] = ke
        toend_ref[:, keys] = to_end
        sloc_ref[keys, :] = dot(ke, v, 0, 0, True)


def forward_kernel(inner_ref, qabs_ref, sin_ref, sloc_ref, a_ref, normed_ref, inv_ref, rounded_ref, send_ref):
    ones = jnp.ones((TOK, 128), f32)
    for h in range(HEADS):
        keys = slice(h * DK, (h + 1) * DK)
        cols = slice(h * DV, (h + 1) * DV)
        s_in = sin_ref[keys, :].astype(f32)
        decay = jnp.exp(dot(a_ref[:, keys], ones, 0, 0, True))[:, 0:1]
        send_ref[keys, :] = decay * s_in + sloc_ref[keys, :]
        raw = inner_ref[:, cols] + dot(qabs_ref[:, keys], s_in, 1, 0, True)
        inv = lax.rsqrt(jnp.mean(raw * raw, axis=1, keepdims=True) + epsilon)
        normed = raw * inv
        normed_ref[:, cols] = normed
        inv_ref[:, keys] = jnp.broadcast_to(inv, (TOK, DK))
        rounded_ref[:, cols] = normed.astype(bf16)


def mixer_kernel(
    place_ref, mine_ref, theirs_ref, w_ref, qabs_ref, normed_ref, inv_ref,
    msg_ref, braw_ref, og0_ref, og1_ref, og2_ref, og3_ref,
):
    core = place_ref[0]
    z = place_ref[1]
    mine = mine_ref[...]
    theirs = theirs_ref[...]
    row_mine = pl.multiple_of(core * HALF, HALF)
    row_theirs = pl.multiple_of((1 - core) * HALF, HALF)
    for h in range(HEADS):
        keys = slice(h * DK, (h + 1) * DK)
        cols = slice(h * DV, (h + 1) * DV)
        bn = dot(mine, w_ref[pl.ds(row_mine, HALF), cols], 1, 0) + dot(
            theirs, w_ref[pl.ds(row_theirs, HALF), cols], 1, 0
        )
        normed = normed_ref[:, cols]
        inv = inv_ref[:, keys][:, 0:1]
        braw = inv * (bn - normed * jnp.mean(bn * normed, axis=1, keepdims=True))
        braw_ref[:, cols] = braw
        msg_ref[keys, :] = dot(qabs_ref[:, keys], braw, 0, 0, True).astype(bf16)
    for shift, ref in enumerate((og0_ref, og1_ref, og2_ref, og3_ref)):
        to = (z + shift) % 4
        cols = pl.ds(pl.multiple_of((to % 2) * HID, HID), HID)
        ref[...] = jnp.where(to // 2 == core, mine_ref[:, cols], theirs_ref[:, cols])


def local_kernel(
    q_ref, k_ref, v_ref, a_ref, sin_ref, braw_ref, qo_ref, dk_ref, dv_ref, dd_ref
):
    for h in range(HEADS):
        r, up, down, q, k, v, qd, ki, scores = forward_parts(q_ref, k_ref, v_ref, a_ref, h)
        rows = slice(h * DK, (h + 1) * DK)
        keys = slice(h * DK, (h + 1) * DK)
        cols = slice(h * DV, (h + 1) * DV)
        s_in = sin_ref[rows, :].astype(f32)
        braw = braw_ref[:, cols]
        vd = jnp.where(tri(True), dot(braw, v, 1, 1, True), 0.0)
        dq = up * dot(vd, ki, 1, 0, True) + jnp.exp(r) * dot(braw, s_in, 1, 1, True)
        dk = down * dot(vd, qd, 0, 0, True)
        dv = dot(scores, braw, 0, 0, True)
        qo_ref[:, keys] = (dq * SCALE).astype(bf16)
        dk_ref[:, keys] = dk
        dv_ref[:, cols] = dv
        dd_ref[:, keys] = q * dq - k * dk


def final_kernel(
    k_ref, v_ref, ke_ref, toend_ref, send_ref, fut_ref, dk_ref, dv_ref, dd_ref, ko_ref, vo_ref, do_ref
):
    upper = tri(False).astype(f32)
    ones_row = jnp.ones((8, DV), f32)
    for h in range(HEADS):
        rows = slice(h * DK, (h + 1) * DK)
        keys = slice(h * DK, (h + 1) * DK)
        cols = slice(h * DV, (h + 1) * DV)
        k = head_cols(k_ref, h, DK)
        fut = fut_ref[rows, :].astype(f32)
        cross = dot(ones_row, send_ref[rows, :] * fut, 1, 1, True)[0:1, :]
        more = toend_ref[:, keys] * dot(v_ref[:, cols], fut_ref[rows, :], 1, 1)
        ko_ref[:, keys] = (dk_ref[:, keys] + more).astype(bf16)
        vo_ref[:, cols] = (dv_ref[:, cols] + dot(ke_ref[:, keys], fut, 1, 0, True)).astype(bf16)
        back = dd_ref[:, keys] - k * more
        do_ref[:, keys] = dot(upper, back, 1, 0, True) + cross


def outer_kernel(*refs):
    total = dot(refs[0][...], refs[4][...], 0, 0)
    for n in range(1, 4):
        total = total + dot(refs[n][...], refs[4 + n][...], 0, 0)
    refs[8][...] = total.astype(bf16)


def total_kernel(terms_ref, out_ref):
    total = terms_ref[0].astype(f32)
    for n in range(1, 16):
        total = total + terms_ref[n].astype(f32)
    out_ref[...] = total


def swapped(x):
    return lax.ppermute(x, "tp", [(0, 1), (1, 0)])


def turned(x, axis, shift):
    return lax.ppermute(x, axis, [(n, (n + shift) % 4) for n in range(4)])


def exchanged(x, axes, count):
    parts = x.reshape(count, x.shape[0] // count, *x.shape[1:])
    return lax.all_to_all(parts, axes, split_axis=0, concat_axis=0, tiled=True).reshape(x.shape)


def body(
    mid_rows,
    cotangent,
    route_experts,
    route_weights,
    gate_weight,
    up_weight,
    down_weight,
    out_weight,
    queries,
    key_rows,
    value_rows,
    log_decay,
):
    return layer(
        mid_rows, cotangent, route_experts, route_weights, gate_weight[0], up_weight[0], down_weight[0],
        out_weight, queries, key_rows, value_rows, log_decay,
    )


def layer(
    mid_rows, cotangent, route_experts, route_weights, gate, up, down,
    out_weight, queries, key_rows, value_rows, log_decay,
):
    core = lax.axis_index("tp").astype(jnp.int32).reshape(1)
    place = jnp.stack([lax.axis_index(n).astype(jnp.int32) for n in ("tp", *SP)])
    ids, wts = route_experts.T, route_weights.T
    mid2, cot2, ids2, wts2 = swapped(mid_rows), swapped(cotangent), swapped(ids), swapped(wts)
    dma = pltpu.SemaphoreType.DMA
    state_msg = call(
        state_kernel, fast((512, SW), bf16), (key_rows, value_rows, log_decay), "ppp", flops=1 << 28
    )
    send, pick = call(
        pack_kernel,
        (far_out((512, MSG), bf16), far_out((512, 2 * ROWS), bf16)),
        (core, ids, ids2, wts, wts2, mid_rows, mid2, cotangent, cot2, state_msg),
        "spnpnfnfnn",
        [pltpu.VMEM((2 * ROWS, D), bf16), pltpu.VMEM((512, D), bf16), pltpu.VMEM((512, 2 * ROWS), bf16), dma((8,))],
        flops=1 << 28,
        manual=(0, 1),
    )
    got = exchanged(send, SP, NDEV)
    keys, values, states = (TOK, 512), (TOK, HALF), (512, DV)
    inner, q_abs, key_end, to_end, state_local = call(
        prior_kernel,
        [far_out(d, f32) for d in (values, keys, keys, keys, states)],
        (queries, key_rows, value_rows, log_decay),
        "pppp",
        flops=1 << 29,
    )
    theirs = swapped(got)

    def scanned(msgs, reverse):
        return call(
            functools.partial(scan_kernel, reverse=reverse),
            far_out(states, bf16),
            (*msgs, got),
            "n" * len(msgs) + "f",
            [pltpu.VMEM((512, SW), bf16)] + [pltpu.VMEM(states, f32)] * 3 + [dma((1,))],
            flops=1 << 26,
        )

    state_out = scanned((), False)
    state_in = exchanged(state_out, SP, NDEV)
    gate, up, down = call(
        load_kernel,
        [fast(w.shape, bf16) for w in (gate, up, down)],
        (gate, up, down),
        "fff",
        [dma((3,))],
        flops=1 << 29,
        limit=2,
        manual=(),
    )
    hid = (512, HID)
    keep, give, hidden, back_gate, back_up = call(
        expert_kernel,
        (fast((512, HALF), bf16), fast((512, HALF), bf16)) + (far_out(hid, bf16),) * 3,
        (core, got, theirs, gate, up, down),
        "sffnnn",
        [pltpu.VMEM((512, D), bf16)] * 2 + [pltpu.VMEM(hid, bf16)] * 3 + [dma((5,))],
        flops=6 << 30,
        limit=24,
        manual=(2, 3, 4),
    )
    back = swapped(give)
    summed = call(return_kernel, far_out((512, HALF), bf16), (keep, back), "nn", flops=1 << 20)
    ret = exchanged(summed, SP, NDEV)
    normed, inv, rounded, state_end = call(
        forward_kernel,
        (far_out(values, f32), far_out(keys, f32), far_out(values, bf16), far_out(states, f32)),
        (inner, q_abs, state_in, state_local, log_decay),
        "ppppp",
        flops=1 << 28,
    )
    normeds = [rounded] + [turned(rounded, "sp_0", n) for n in range(1, 4)]
    token_mine = call(
        combine_kernel,
        fast(values, bf16),
        (core, pick, ret, cotangent, cot2),
        "spnpp",
        flops=1 << 26,
    )
    token_theirs = swapped(token_mine)
    (near_weight,) = call(
        load_kernel,
        [fast(out_weight.shape, bf16)],
        (out_weight,),
        "f",
        [dma((1,))],
        flops=1 << 29,
        limit=2,
    )
    back_msg, braw, *columns = call(
        mixer_kernel,
        (far_out(states, bf16), far_out(values, f32)) + (far_out((TOK, HID), bf16),) * 4,
        (place, token_mine, token_theirs, near_weight, q_abs, normed, inv),
        "snnnppp",
        flops=1 << 30,
    )
    back_got = exchanged(back_msg, SP, NDEV)
    columns = columns[:1] + [turned(columns[n], "sp_0", n) for n in range(1, 4)]
    state_back = scanned((back_got,), True)
    future = exchanged(state_back, SP, NDEV)
    query_out, dk_part, dv_part, dd_part = call(
        local_kernel,
        (far_out(keys, bf16), far_out(keys, f32), far_out(values, f32), far_out(keys, f32)),
        (queries, key_rows, value_rows, log_decay, state_in, braw),
        "pppppp",
        flops=1 << 30,
    )
    outer = call(outer_kernel, far_out((512, HALF), bf16), (*columns, *normeds), "pnnnpppp", flops=1 << 29)
    terms = lax.all_to_all(
        outer.reshape(16, 32, HALF), ("sp_1", "sp_2"), split_axis=0, concat_axis=0, tiled=True
    )
    key_out, value_out, decay_out = call(
        final_kernel,
        (far_out(keys, bf16), far_out(values, bf16), far_out(keys, f32)),
        (key_rows, value_rows, key_end, to_end, state_end, future, dk_part, dv_part, dd_part),
        "pppppnppp",
        flops=1 << 29,
    )
    gate_total, up_total, down_total = call(
        grads_kernel,
        (far_out((D, HID), bf16), far_out((D, HID), bf16), far_out((HID, D), bf16)),
        (core, got, theirs, hidden, back_gate, back_up),
        "sffppp",
        [pltpu.VMEM((512, D), bf16)] * 2 + [dma((2,))],
        flops=3 << 30,
        limit=28,
    )
    out_total = call(total_kernel, far_out((32, HALF), f32), (terms,), "n", flops=1 << 20)
    totals = (gate_total[None], up_total[None], down_total[None])
    return (*totals, out_total, query_out, key_out, value_out, decay_out)


def solution(mesh):
    split = Mesh(mesh.devices.reshape(4, 4, 4, mesh.shape["tp"]), ("sp_0", "sp_1", "sp_2", "tp"))
    placed = (
        P(SP_TP, None),
        P(SP_TP, None),
        P(SP_TP, None),
        P(SP_TP, None),
        P(SP, None, "tp"),
        P(SP, None, "tp"),
        P(SP, "tp", None),
        P(None, "tp"),
        P(SP, "tp"),
        P(SP, "tp"),
        P(SP, "tp"),
        P(SP, "tp"),
    )
    return jax.shard_map(
        body,
        mesh=split,
        in_specs=placed,
        out_specs=(
            P(SP, None, "tp"),
            P(SP, None, "tp"),
            P(SP, "tp", None),
            P(SP, "tp"),
            P(SP, "tp"),
            P(SP, "tp"),
            P(SP, "tp"),
            P(SP, "tp"),
        ),
        check_vma=False,
    )
```

```python
import functools

import jax
import jax.numpy as jnp
from jax import lax
from jax.experimental import pallas as pl
from jax.experimental.pallas import tpu as pltpu
from jax.sharding import Mesh
from jax.sharding import PartitionSpec as P


DK = 128
DV = 256
SP = ("sp_0", "sp_1", "sp_2")
SP_TP = ("sp_0", "sp_1", "sp_2", "tp")
ROWS = 64
D = 2048
HALF = 1024
HID = 512
HEADS = 4
TOK = 128
NDEV = 64
SW = DV + 128
MSG = SW + D
SCALE = DK**-0.5


f32 = jnp.float32
bf16 = jnp.bfloat16
epsilon = 1e-06


def dot(a, b, ca, cb, high=False):
    return lax.dot_general(
        a,
        b,
        (((ca,), (cb,)), ((), ())),
        precision=lax.Precision.HIGHEST if high else None,
        preferred_element_type=f32,
    )


def fast(dims, dtype):
    return pltpu.VMEM(dims, dtype)


def pieces(x, count):
    out = []
    for _ in range(count):
        out.append(x.astype(bf16))
        x = x - out[-1].astype(f32)
    return out


def wide_narrow(a, b, ca, cb, count=2):
    return sum(dot(p, b, ca, cb) for p in reversed(pieces(a, count)))


def narrow_wide(a, b, ca, cb, count=2):
    return sum(dot(a, p, ca, cb) for p in reversed(pieces(b, count)))


def wide_wide(a, b, ca, cb):
    a0, a1 = pieces(a, 2)
    b0, b1 = pieces(b, 2)
    return dot(a1, b0, ca, cb) + dot(a0, b1, ca, cb) + dot(a0, b0, ca, cb)


def far_out(dims, dtype):
    return pltpu.HBM(dims, dtype)


SMEM, NEAR, FAR = "s", "n", "f"


def call(kernel, out_shape, args, kinds, scratch=(), flops=0, limit=12, manual=()):
    vmem = pl.BlockSpec(memory_space=pltpu.VMEM)
    specs = {SMEM: pl.BlockSpec(memory_space=pltpu.SMEM), FAR: pl.BlockSpec(memory_space=pl.ANY)}
    spaces = {NEAR: pltpu.VMEM, FAR: pltpu.HBM}
    many = isinstance(out_shape, (list, tuple))
    outs = list(out_shape) if many else [out_shape]
    out_specs = [specs[FAR] if i in manual else vmem for i in range(len(outs))]
    args = [
        pltpu.with_memory_space_constraint(a, spaces[k]) if k in spaces else a for a, k in zip(args, kinds)
    ]
    return pl.pallas_call(
        kernel,
        out_shape=out_shape,
        in_specs=[specs.get(k, vmem) for k in kinds],
        out_specs=out_specs if many else out_specs[0],
        scratch_shapes=list(scratch),
        compiler_params=pltpu.CompilerParams(vmem_limit_bytes=limit * 1024 * 1024),
        cost_estimate=pl.CostEstimate(flops=flops, transcendentals=0, bytes_accessed=1 << 20),
    )(*args)


def tri(lower):
    i = lax.broadcasted_iota(jnp.int32, (TOK, TOK), 0)
    j = lax.broadcasted_iota(jnp.int32, (TOK, TOK), 1)
    return (i >= j) if lower else (i <= j)


def head_cols(ref, h, width):
    return ref[:, h * width : (h + 1) * width].astype(f32)


def state_rows(k_ref, v_ref, a_ref, msg_ref):
    lower = tri(True).astype(bf16)
    ones = jnp.ones((TOK, 128), bf16)
    lane = lax.broadcasted_iota(jnp.int32, (DK, 128), 1)
    for h in range(HEADS):
        a = head_cols(a_ref, h, DK)
        r = narrow_wide(lower, a, 1, 0, 3)
        ke = head_cols(k_ref, h, DK) * jnp.exp(r[TOK - 1 :, :] - r)
        s = wide_narrow(ke, v_ref[:, h * DV : (h + 1) * DV], 0, 0)
        rows = slice(h * DK, (h + 1) * DK)
        msg_ref[rows, 0:DV] = s.astype(bf16)
        col = wide_narrow(a, ones, 0, 0, 3)
        hi = col.astype(bf16).astype(f32)
        mid = (col - hi).astype(bf16).astype(f32)
        lo = col - hi - mid
        part = jnp.where(lane == 0, hi, jnp.where(lane == 1, mid, jnp.where(lane == 2, lo, 0.0)))
        msg_ref[rows, DV:SW] = part.astype(bf16)


def pack_kernel(
    core_ref, ids_hbm, ids2_ref, wts_hbm, wts2_ref, mid_ref, mid2_ref, cot_ref, cot2_ref, k_hbm, v_hbm, a_hbm,
    out_ref, pick_ref, ids_ref, wts_ref, k_ref, v_ref, a_ref, state_ref, rows_ref, send_ref, pick_v_ref, sems,
):
    core = core_ref[0]
    pairs = ((a_hbm, a_ref), (k_hbm, k_ref), (v_hbm, v_ref), (ids_hbm, ids_ref), (wts_hbm, wts_ref))
    fetches = [pltpu.make_async_copy(src, dst, sems.at[8 + i]) for i, (src, dst) in enumerate(pairs)]
    for c in reversed(fetches):
        c.start()

    @pl.when(core == 0)
    def _():
        pltpu.make_async_copy(mid_ref, rows_ref.at[0:ROWS], sems.at[0]).start()
        pltpu.make_async_copy(mid2_ref, rows_ref.at[ROWS : 2 * ROWS], sems.at[1]).start()

    @pl.when(core == 1)
    def _():
        pltpu.make_async_copy(cot_ref, rows_ref.at[0:ROWS], sems.at[0]).start()
        pltpu.make_async_copy(cot2_ref, rows_ref.at[ROWS : 2 * ROWS], sems.at[1]).start()

    for c in fetches[3:]:
        c.wait()
    expert = lax.broadcasted_iota(jnp.int32, (NDEV, ROWS), 0)
    ti = lax.broadcasted_iota(jnp.int32, (ROWS, ROWS), 0)
    tj = lax.broadcasted_iota(jnp.int32, (ROWS, ROWS), 1)
    before = (ti < tj).astype(bf16)
    si = lax.broadcasted_iota(jnp.int32, (8 * NDEV, NDEV), 0)
    se = lax.broadcasted_iota(jnp.int32, (8 * NDEV, NDEV), 1)
    expand = (si // 8 == se).astype(bf16)
    slot = (si % 4 + 1).astype(f32)
    owner = (si % 8) // 4

    def picks(ids, wts, which):
        e1 = (ids[0:1, :] == expert).astype(f32)
        e2 = (ids[1:2, :] == expert).astype(f32)
        both = e1 + e2
        rank = both * (dot(both.astype(bf16), before, 1, 0) + 1.0)
        weight = e1 * wts[0:1, :] + e2 * wts[1:2, :]
        found = dot(expand, rank.astype(bf16), 1, 0)
        return jnp.where((found == slot) & (owner == which), 1.0, 0.0), weight

    own, weight_own = picks(ids_ref, wts_ref, core)
    other, weight_other = picks(ids2_ref, wts2_ref, 1 - core)
    pick_v_ref[:, 0:ROWS] = own.astype(bf16)
    pick_v_ref[:, ROWS:] = other.astype(bf16)
    pick_out = pltpu.make_async_copy(pick_v_ref, pick_ref, sems.at[2])
    pick_out.start()
    w = own * narrow_wide(expand, weight_own, 1, 0, 3) + other * narrow_wide(expand, weight_other, 1, 0, 3)
    scale = jnp.where(core == 0, 1.0, jnp.sum(w, axis=1, keepdims=True))
    pltpu.make_async_copy(mid_ref, rows_ref.at[0:ROWS], sems.at[0]).wait()
    pltpu.make_async_copy(mid2_ref, rows_ref.at[ROWS : 2 * ROWS], sems.at[1]).wait()
    outs = []
    for i in range(4):
        cols = slice(i * HID, (i + 1) * HID)
        rows = dot(pick_v_ref[...], rows_ref[:, cols], 1, 0)
        send_ref[:, cols] = (rows * scale).astype(bf16)
        to = out_ref.at[:, SW + i * HID : SW + (i + 1) * HID]
        outs.append(pltpu.make_async_copy(send_ref.at[:, cols], to, sems.at[3 + i]))
        outs[i].start()
    for c in fetches[:3]:
        c.wait()
    state_rows(k_ref, v_ref, a_ref, state_ref)
    state_out = pltpu.make_async_copy(state_ref, out_ref.at[:, 0:SW], sems.at[7])
    state_out.start()
    pick_out.wait()
    state_out.wait()
    for c in outs:
        c.wait()


def fetch_parts(core, first_ref, second_ref, to_ref, sems):
    def parts(ref):
        return [
            pltpu.make_async_copy(
                ref.at[:, SW + i * HID : SW + (i + 1) * HID], to_ref.at[:, i * HID : (i + 1) * HID], sems.at[i]
            )
            for i in range(4)
        ]

    for which, ref in enumerate((first_ref, second_ref)):

        @pl.when(core == which)
        def _():
            for c in parts(ref):
                c.start()

    return parts(first_ref)


def down_kernel(core_ref, got_ref, other_ref, hidden_hbm, down_hbm, scaled_ref, hidden_ref, down_ref, sems):
    hidden_in = pltpu.make_async_copy(hidden_hbm, hidden_ref, sems.at[4])
    hidden_in.start()
    fetches = fetch_parts(core_ref[0], other_ref, got_ref, scaled_ref, sems)
    hidden_in.wait()
    copies = []
    for i in range(4):
        part = slice(i * HID, (i + 1) * HID)
        fetches[i].wait()
        down_ref[:, part] = dot(hidden_ref[...], scaled_ref[:, part], 0, 0).astype(bf16)
        copies.append(pltpu.make_async_copy(down_ref.at[:, part], down_hbm.at[:, part], sems.at[5 + i]))
        copies[i].start()
    for c in copies:
        c.wait()


def grads_kernel(
    core_ref, got_ref, other_ref, bg_hbm, bu_hbm, gate_hbm, up_hbm, rows_ref, bg_ref, bu_ref, gate_ref, up_ref, sems
):
    bg_in = pltpu.make_async_copy(bg_hbm, bg_ref, sems.at[4])
    bu_in = pltpu.make_async_copy(bu_hbm, bu_ref, sems.at[5])
    bg_in.start()
    fetches = fetch_parts(core_ref[0], got_ref, other_ref, rows_ref, sems)
    bu_in.start()
    bg_in.wait()
    copies = []
    for i in range(4):
        part = slice(i * HID, (i + 1) * HID)
        fetches[i].wait()
        x = rows_ref[:, part]
        gate_ref[part, :] = dot(x, bg_ref[...], 0, 0).astype(bf16)
        copies.append(pltpu.make_async_copy(gate_ref.at[part], gate_hbm.at[part], sems.at[6 + 2 * i]))
        copies[-1].start()
        if i == 0:
            bu_in.wait()
        up_ref[part, :] = dot(x, bu_ref[...], 0, 0).astype(bf16)
        copies.append(pltpu.make_async_copy(up_ref.at[part], up_hbm.at[part], sems.at[7 + 2 * i]))
        copies[-1].start()
    for c in copies:
        c.wait()


def load_kernel(*refs, start=0):
    count = (len(refs) - 1) // 2
    copies = [
        pltpu.make_async_copy(refs[i].at[start : start + refs[count + i].shape[0]], refs[count + i], refs[-1].at[i])
        for i in range(count)
    ]
    for c in copies:
        c.start()
    for c in copies:
        c.wait()


def scan_steps(out_ref, x_ref, d_ref, y_ref, reverse):
    state = jnp.zeros((8, DV), f32)
    for n in range(NDEV):
        p = NDEV - 1 - n if reverse else n
        rows = slice(8 * p, 8 * p + 8)
        y_ref[rows, :] = state
        state = d_ref[rows, :] * state + x_ref[rows, :]
    out_ref[...] = y_ref[...].astype(bf16)


def scan_in_kernel(got_ref, out_ref, d_ref, part_ref, x_ref, y_ref, sem):
    copy = pltpu.make_async_copy(got_ref.at[:, 0:SW], part_ref, sem.at[0])
    copy.start()
    copy.wait()
    x_ref[...] = part_ref[:, 0:DV].astype(f32)
    log = jnp.sum(part_ref[:, DV:].astype(f32), axis=1, keepdims=True)
    d_ref[...] = jnp.broadcast_to(jnp.exp(log), (8 * NDEV, DV))
    scan_steps(out_ref, x_ref, d_ref, y_ref, False)


def scan_back_kernel(msg_ref, d_ref, out_ref, x_ref, y_ref):
    x_ref[...] = msg_ref[...].astype(f32)
    scan_steps(out_ref, x_ref, d_ref, y_ref, True)


def expert_kernel(
    core_ref, mine_ref, theirs_ref, gate_ref, up_hbm, down_hbm,
    send_ref, bg_ref, bu_ref, up_ref, hidden_out, bg_out, bu_out,
    rows_ref, scaled_ref, hidden_ref, down_ref, sems,
):
    core = core_ref[0]
    mine_ref = mine_ref.at[:, SW:MSG]
    theirs_ref = theirs_ref.at[:, SW:MSG]
    up_in = pltpu.make_async_copy(up_hbm, up_ref, sems.at[5])
    down_in = pltpu.make_async_copy(down_hbm, down_ref, sems.at[6])

    @pl.when(core == 0)
    def _():
        pltpu.make_async_copy(mine_ref, rows_ref, sems.at[0]).start()

    @pl.when(core == 1)
    def _():
        pltpu.make_async_copy(theirs_ref, rows_ref, sems.at[0]).start()

    up_in.start()

    @pl.when(core == 0)
    def _():
        pltpu.make_async_copy(theirs_ref, scaled_ref, sems.at[1]).start()

    @pl.when(core == 1)
    def _():
        pltpu.make_async_copy(mine_ref, scaled_ref, sems.at[1]).start()

    down_in.start()
    pltpu.make_async_copy(mine_ref, rows_ref, sems.at[0]).wait()
    pre_gate = dot(rows_ref[...], gate_ref[...], 1, 0)
    up_in.wait()
    pre_up = dot(rows_ref[...], up_ref[...], 1, 0)
    sig = 1.0 / (1.0 + jnp.exp(-pre_gate))
    swish = pre_gate * sig
    slope = sig * (1.0 + pre_gate * (1.0 - sig))
    hidden_ref[...] = (swish * pre_up).astype(bf16)
    hidden_copy = pltpu.make_async_copy(hidden_ref, hidden_out, sems.at[2])
    hidden_copy.start()
    pltpu.make_async_copy(mine_ref, scaled_ref, sems.at[1]).wait()
    down_in.wait()
    back = dot(scaled_ref[...], down_ref[...], 1, 1)
    bg_ref[...] = (back * pre_up * slope).astype(bf16)
    bu_ref[...] = (back * swish).astype(bf16)
    bg_copy = pltpu.make_async_copy(bg_ref, bg_out, sems.at[3])
    bu_copy = pltpu.make_async_copy(bu_ref, bu_out, sems.at[4])
    bg_copy.start()
    bu_copy.start()

    send_ref[...] = half_rows(1 - core, bg_ref, bu_ref, gate_ref, up_ref)
    for c in (hidden_copy, bg_copy, bu_copy):
        c.wait()


def half_rows(c, bg_ref, bu_ref, gate_ref, up_ref):
    cols = pl.ds(pl.multiple_of(c * HALF, HALF), HALF)
    return (dot(bg_ref[...], gate_ref[cols, :], 1, 1) + dot(bu_ref[...], up_ref[cols, :], 1, 1)).astype(bf16)


def keep_kernel(core_ref, bg_ref, bu_ref, gate_ref, up_ref, keep_ref):
    keep_ref[...] = half_rows(core_ref[0], bg_ref, bu_ref, gate_ref, up_ref)


def return_kernel(keep_ref, got_ref, out_ref):
    out_ref[...] = (keep_ref[...].astype(f32) + got_ref[...].astype(f32)).astype(bf16)


def combine_kernel(core_ref, pick_hbm, ret_ref, cot_hbm, cot2_hbm, out_ref, pick_ref, cot_ref, cot2_ref, sems):
    core = core_ref[0]
    cols = pl.ds(pl.multiple_of(core * HALF, HALF), HALF)
    pairs = ((pick_hbm, pick_ref), (cot_hbm.at[:, cols], cot_ref), (cot2_hbm.at[:, cols], cot2_ref))
    copies = [pltpu.make_async_copy(src, dst, sems.at[i]) for i, (src, dst) in enumerate(pairs)]
    for c in copies:
        c.start()
    copies[0].wait()
    rows = dot(pick_ref[...], ret_ref[...], 0, 0)
    copies[1].wait()
    copies[2].wait()

    def put(picked, cot, which):
        total = picked + cot[...].astype(f32)
        out_ref[pl.ds(pl.multiple_of(which * ROWS, ROWS), ROWS), :] = total.astype(bf16)

    put(rows[0:ROWS], cot_ref, core)
    put(rows[ROWS:], cot2_ref, 1 - core)


def decayed(q_ref, k_ref, a_ref, h):
    r = narrow_wide(tri(True).astype(bf16), head_cols(a_ref, h, DK), 1, 0, 3)
    mid = r[TOK // 2 : TOK // 2 + 1, :]
    up = jnp.exp(r - mid)
    down = jnp.exp(mid - r)
    q = head_cols(q_ref, h, DK) * SCALE
    k = head_cols(k_ref, h, DK)
    return r, up, down, q, k, q * up, k * down


def prior_kernel(q_ref, k_ref, v_ref, a_ref, inner_ref, qabs_ref, ke_ref, toend_ref, scores_ref, sloc_ref):
    for h in range(HEADS):
        r, _, _, q, k, qd, ki = decayed(q_ref, k_ref, a_ref, h)
        v = v_ref[:, h * DV : (h + 1) * DV]
        keys = slice(h * DK, (h + 1) * DK)
        scores = jnp.where(tri(True), wide_wide(qd, ki, 1, 1), 0.0)
        scores_ref[:, keys] = scores
        inner_ref[:, h * DV : (h + 1) * DV] = wide_narrow(scores, v, 1, 0)
        qabs_ref[:, keys] = q * jnp.exp(r)
        to_end = jnp.exp(r[TOK - 1 :, :] - r)
        ke = k * to_end
        ke_ref[:, keys] = ke
        toend_ref[:, keys] = to_end
        sloc_ref[keys, :] = wide_narrow(ke, v, 0, 0)


def forward_kernel(inner_ref, qabs_ref, sin_ref, sloc_ref, a_ref, normed_ref, inv_ref, rounded_ref, send_ref):
    ones = jnp.ones((TOK, 128), bf16)
    for h in range(HEADS):
        keys = slice(h * DK, (h + 1) * DK)
        cols = slice(h * DV, (h + 1) * DV)
        decay = jnp.exp(wide_narrow(a_ref[:, keys], ones, 0, 0, 3))[:, 0:1]
        send_ref[keys, :] = decay * sin_ref[keys, :].astype(f32) + sloc_ref[keys, :]
        raw = inner_ref[:, cols] + wide_narrow(qabs_ref[:, keys], sin_ref[keys, :], 1, 0)
        inv = lax.rsqrt(jnp.mean(raw * raw, axis=1, keepdims=True) + epsilon)
        normed = raw * inv
        normed_ref[:, cols] = normed
        inv_ref[:, keys] = jnp.broadcast_to(inv, (TOK, DK))
        rounded_ref[:, cols] = normed.astype(bf16)


def mixer_kernel(
    place_ref, mine_ref, theirs_ref, w0_ref, w1_ref, qabs_ref, normed_ref, inv_ref,
    msg_ref, braw_ref, og0_ref, og1_ref, og2_ref, og3_ref,
):
    core = place_ref[0]
    z = place_ref[1]
    mine = mine_ref[...]
    theirs = theirs_ref[...]
    first = jnp.where(core == 0, mine, theirs)
    second = jnp.where(core == 0, theirs, mine)
    for h in range(HEADS):
        keys = slice(h * DK, (h + 1) * DK)
        cols = slice(h * DV, (h + 1) * DV)
        bn = dot(first, w0_ref[:, cols], 1, 0) + dot(second, w1_ref[:, cols], 1, 0)
        normed = normed_ref[:, cols]
        inv = inv_ref[:, keys][:, 0:1]
        braw = inv * (bn - normed * jnp.mean(bn * normed, axis=1, keepdims=True))
        braw_ref[:, cols] = braw
        msg_ref[keys, :] = wide_wide(qabs_ref[:, keys], braw, 0, 0).astype(bf16)
    for shift, ref in enumerate((og0_ref, og1_ref, og2_ref, og3_ref)):
        to = (z + shift) % 4
        cols = pl.ds(pl.multiple_of((to % 2) * HID, HID), HID)
        ref[...] = jnp.where(to // 2 == core, mine_ref[:, cols], theirs_ref[:, cols])


def local_kernel(
    q_ref, k_ref, v_ref, a_ref, sin_ref, braw_ref, scores_ref, qo_ref, dk_ref, dv_ref, dd_ref
):
    for h in range(HEADS):
        r, up, down, q, k, qd, ki = decayed(q_ref, k_ref, a_ref, h)
        keys = slice(h * DK, (h + 1) * DK)
        cols = slice(h * DV, (h + 1) * DV)
        braw = braw_ref[:, cols]
        vd = jnp.where(tri(True), wide_narrow(braw, v_ref[:, cols], 1, 1), 0.0)
        dq = up * wide_wide(vd, ki, 1, 0) + jnp.exp(r) * wide_narrow(braw, sin_ref[keys, :], 1, 1)
        dk = down * wide_wide(vd, qd, 0, 0)
        dv = wide_wide(scores_ref[:, keys], braw, 0, 0)
        qo_ref[:, keys] = (dq * SCALE).astype(bf16)
        dk_ref[:, keys] = dk
        dv_ref[:, cols] = dv
        dd_ref[:, keys] = q * dq - k * dk


def final_kernel(
    k_ref, v_ref, ke_ref, toend_ref, send_ref, fut_ref, dk_ref, dv_ref, dd_ref, ko_ref, vo_ref, do_ref
):
    upper = tri(False).astype(bf16)
    ones_row = jnp.ones((8, DV), bf16)
    for h in range(HEADS):
        rows = slice(h * DK, (h + 1) * DK)
        keys = slice(h * DK, (h + 1) * DK)
        cols = slice(h * DV, (h + 1) * DV)
        fut = fut_ref[rows, :]
        cross = narrow_wide(ones_row, send_ref[rows, :] * fut.astype(f32), 1, 1, 3)[0:1, :]
        more = toend_ref[:, keys] * dot(v_ref[:, cols], fut, 1, 1)
        ko_ref[:, keys] = (dk_ref[:, keys] + more).astype(bf16)
        vo_ref[:, cols] = (dv_ref[:, cols] + wide_narrow(ke_ref[:, keys], fut, 1, 0)).astype(bf16)
        back = dd_ref[:, keys] - head_cols(k_ref, h, DK) * more
        do_ref[:, keys] = narrow_wide(upper, back, 1, 0, 3) + cross


def outer_kernel(*refs):
    total = dot(refs[0][...], refs[4][...], 0, 0)
    for n in range(1, 4):
        total = total + dot(refs[n][...], refs[4 + n][...], 0, 0)
    refs[8][...] = total.astype(bf16)


def total_kernel(terms_ref, out_ref):
    total = terms_ref[0].astype(f32)
    for n in range(1, 16):
        total = total + terms_ref[n].astype(f32)
    out_ref[...] = total


def swapped(x):
    return lax.ppermute(x, "tp", [(0, 1), (1, 0)])


def turned(x, axis, shift):
    return lax.ppermute(x, axis, [(n, (n + shift) % 4) for n in range(4)])


def exchanged(x, axes, count):
    parts = x.reshape(count, x.shape[0] // count, *x.shape[1:])
    return lax.all_to_all(parts, axes, split_axis=0, concat_axis=0, tiled=True).reshape(x.shape)


def body(
    mid_rows,
    cotangent,
    route_experts,
    route_weights,
    gate_weight,
    up_weight,
    down_weight,
    out_weight,
    queries,
    key_rows,
    value_rows,
    log_decay,
):
    return layer(
        mid_rows, cotangent, route_experts, route_weights, gate_weight[0], up_weight[0], down_weight[0],
        out_weight, queries, key_rows, value_rows, log_decay,
    )


def layer(
    mid_rows, cotangent, route_experts, route_weights, gate, up, down,
    out_weight, queries, key_rows, value_rows, log_decay,
):
    core = lax.axis_index("tp").astype(jnp.int32).reshape(1)
    place = jnp.stack([lax.axis_index(n).astype(jnp.int32) for n in ("tp", *SP)])
    ids, wts = route_experts.T, route_weights.T
    mid2, cot2, ids2, wts2 = swapped(mid_rows), swapped(cotangent), swapped(ids), swapped(wts)
    dma = pltpu.SemaphoreType.DMA

    def loaded(*arrays, start=0, rows=None):
        return call(
            functools.partial(load_kernel, start=start),
            [fast((rows or w.shape[0], w.shape[1]), bf16) for w in arrays],
            arrays,
            "f" * len(arrays),
            [dma((len(arrays),))],
            flops=1 << 29,
            limit=2,
        )

    send, pick = call(
        pack_kernel,
        (far_out((512, MSG), bf16), far_out((512, 2 * ROWS), bf16)),
        (core, ids, ids2, wts, wts2, mid_rows, mid2, cotangent, cot2, key_rows, value_rows, log_decay),
        "sfnfnfnfnfff",
        [
            pltpu.VMEM((2, ROWS), jnp.int32), pltpu.VMEM((2, ROWS), f32), pltpu.VMEM((TOK, 512), bf16),
            pltpu.VMEM((TOK, HALF), bf16), pltpu.VMEM((TOK, 512), f32), pltpu.VMEM((512, SW), bf16),
            pltpu.VMEM((2 * ROWS, D), bf16), pltpu.VMEM((512, D), bf16), pltpu.VMEM((512, 2 * ROWS), bf16), dma((13,)),
        ],
        flops=1 << 28,
        manual=(0, 1),
    )
    got = exchanged(send, SP, NDEV)
    keys, values, states = (TOK, 512), (TOK, HALF), (512, DV)
    inner, q_abs, key_end, to_end, scores, state_local = call(
        prior_kernel,
        [far_out(d, f32) for d in (values, keys, keys, keys, keys, states)],
        (queries, key_rows, value_rows, log_decay),
        "pppp",
        flops=1 << 29,
    )
    theirs = swapped(got)

    wide_states = pltpu.VMEM(states, f32)
    state_out, decays = call(
        scan_in_kernel,
        (far_out(states, bf16), far_out(states, f32)),
        (got,),
        "f",
        [pltpu.VMEM((512, SW), bf16), wide_states, wide_states, dma((1,))],
        flops=1 << 26,
    )
    state_in = exchanged(state_out, SP, NDEV)
    (gate,) = loaded(gate)
    hid = (512, HID)
    give, near_gate, near_up, up, hidden, back_gate, back_up = call(
        expert_kernel,
        (fast((512, HALF), bf16), fast(hid, bf16), fast(hid, bf16), fast(up.shape, bf16)) + (far_out(hid, bf16),) * 3,
        (core, got, theirs, gate, up, down),
        "sffnff",
        [pltpu.VMEM((512, D), bf16)] * 2 + [pltpu.VMEM(hid, bf16), pltpu.VMEM(down.shape, bf16), dma((7,))],
        flops=6 << 30,
        limit=24,
        manual=(4, 5, 6),
    )
    back = swapped(give)
    keep = call(keep_kernel, fast((512, HALF), bf16), (core, near_gate, near_up, gate, up), "snnnn", flops=1 << 30)
    summed = call(return_kernel, far_out((512, HALF), bf16), (keep, back), "nn", flops=1 << 20)
    ret = exchanged(summed, SP, NDEV)
    normed, inv, rounded, state_end = call(
        forward_kernel,
        (far_out(values, f32), far_out(keys, f32), far_out(values, bf16), far_out(states, f32)),
        (inner, q_abs, state_in, state_local, log_decay),
        "ppppp",
        flops=1 << 28,
    )
    normeds = [rounded, turned(rounded, "sp_0", 1), None, turned(rounded, "sp_0", 3)]
    normeds[2] = turned(normeds[3], "sp_0", 3)
    token_mine = call(
        combine_kernel,
        fast(values, bf16),
        (core, pick, ret, cotangent, cot2),
        "sfnff",
        [pltpu.VMEM((512, 2 * ROWS), bf16), pltpu.VMEM((ROWS, HALF), bf16), pltpu.VMEM((ROWS, HALF), bf16), dma((3,))],
        flops=1 << 26,
    )
    token_theirs = swapped(token_mine)
    (first_weight,) = loaded(out_weight, rows=HALF)
    (second_weight,) = loaded(out_weight, start=HALF, rows=HALF)
    back_msg, braw, *columns = call(
        mixer_kernel,
        (far_out(states, bf16), far_out(values, f32)) + (far_out((TOK, HID), bf16),) * 4,
        (place, token_mine, token_theirs, first_weight, second_weight, q_abs, normed, inv),
        "snnnnppp",
        flops=1 << 30,
    )
    back_got = exchanged(back_msg, SP, NDEV)
    columns = columns[:1] + [turned(columns[n], "sp_0", n) for n in range(1, 4)]
    state_back = call(
        scan_back_kernel, far_out(states, bf16), (back_got, decays), "np", [wide_states, wide_states], flops=1 << 26
    )
    future = exchanged(state_back, SP, NDEV)
    query_out, dk_part, dv_part, dd_part = call(
        local_kernel,
        (far_out(keys, bf16), far_out(keys, f32), far_out(values, f32), far_out(keys, f32)),
        (queries, key_rows, value_rows, log_decay, state_in, braw, scores),
        "ppppppp",
        flops=1 << 30,
    )
    outer = call(outer_kernel, far_out((512, HALF), bf16), (*columns, *normeds), "pnnnpppp", flops=1 << 29)
    terms = lax.all_to_all(
        outer.reshape(16, 32, HALF), ("sp_1", "sp_2"), split_axis=0, concat_axis=0, tiled=True
    )
    key_out, value_out, decay_out = call(
        final_kernel,
        (far_out(keys, bf16), far_out(values, bf16), far_out(keys, f32)),
        (key_rows, value_rows, key_end, to_end, state_end, future, dk_part, dv_part, dd_part),
        "pppppnppp",
        flops=1 << 29,
    )
    down_total = call(
        down_kernel,
        far_out((HID, D), bf16),
        (core, got, theirs, hidden),
        "sfff",
        [pltpu.VMEM((512, D), bf16), pltpu.VMEM(hid, bf16), pltpu.VMEM((HID, D), bf16), dma((9,))],
        flops=1 << 30,
        manual=(0,),
    )
    gate_total, up_total = call(
        grads_kernel,
        (far_out((D, HID), bf16), far_out((D, HID), bf16)),
        (core, got, theirs, back_gate, back_up),
        "sffff",
        [pltpu.VMEM((512, D), bf16), pltpu.VMEM(hid, bf16), pltpu.VMEM(hid, bf16)]
        + [pltpu.VMEM((D, HID), bf16)] * 2
        + [dma((14,))],
        flops=2 << 30,
        limit=20,
        manual=(0, 1),
    )
    out_total = call(total_kernel, far_out((32, HALF), f32), (terms,), "n", flops=1 << 20)
    totals = (gate_total[None], up_total[None], down_total[None])
    return (*totals, out_total, query_out, key_out, value_out, decay_out)


def solution(mesh):
    split = Mesh(mesh.devices.reshape(4, 4, 4, mesh.shape["tp"]), ("sp_0", "sp_1", "sp_2", "tp"))
    placed = (
        P(SP_TP, None),
        P(SP_TP, None),
        P(SP_TP, None),
        P(SP_TP, None),
        P(SP, None, "tp"),
        P(SP, None, "tp"),
        P(SP, "tp", None),
        P(None, "tp"),
        P(SP, "tp"),
        P(SP, "tp"),
        P(SP, "tp"),
        P(SP, "tp"),
    )
    return jax.shard_map(
        body,
        mesh=split,
        in_specs=placed,
        out_specs=(
            P(SP, None, "tp"),
            P(SP, None, "tp"),
            P(SP, "tp", None),
            P(SP, "tp"),
            P(SP, "tp"),
            P(SP, "tp"),
            P(SP, "tp"),
            P(SP, "tp"),
        ),
        check_vma=False,
    )
```
